32 devices in a mesh: sp: 8 (over z, x), tp: 4 (over y, core).
Axes of the slice: x: 2, y: 2, z: 4, core: 2. Of those that a mesh axis runs over, the one named last changes fastest.
Arguments:
- queries_one: bfloat16 [1024, 2048], P('sp', 'tp'), may hold values from -6.2 to 6.2
- keys_one: bfloat16 [1024, 2048], P('sp', 'tp'), may hold values from -5 to 5
- values_one: bfloat16 [1024, 2048], P('sp', 'tp'), may hold values from -6 to 6
- queries_two: bfloat16 [1024, 1024], P('sp', 'tp'), may hold values from -6.2 to 6.2
- keys_two: bfloat16 [1024, 1024], P('sp', 'tp'), may hold values from -5 to 5
- values_two: bfloat16 [1024, 1024], P('sp', 'tp'), may hold values from -6 to 6
- key_offset: bfloat16 [1024, 2, 16], P('sp', None, 'tp'), may hold values from -14 to 0
- out_one: bfloat16 [2048, 4096], P('tp'), may hold values from -0.109375 to 0.109375
- out_two: bfloat16 [1024, 4096], P('tp'), may hold values from -0.109375 to 0.109375
- residual: bfloat16 [1024, 4096], P('sp', 'tp'), may hold values from -6 to 6
- norm_gain: float32 [4096], replicated, may hold values from 0.1 to 1.9
- routes: int32 [1024, 2], P('sp'), may hold values from 0 to 7, all different within a row; in each aligned block of 128 rows (0 to 127, 128 to 255, ...) at most 64 rows name the same one
- route_weight: float32 [1024, 2], P('sp'), may hold values from 0.2 to 1
- expert_gate: bfloat16 [8, 4096, 2048], P('sp', None, 'tp'), may hold values from -0.09375 to 0.09375
- expert_up: bfloat16 [8, 4096, 2048], P('sp', None, 'tp'), may hold values from -0.09375 to 0.09375
- expert_down: bfloat16 [8, 2048, 4096], P('sp', None, 'tp'), may hold values from -0.125 to 0.125
Outputs:
- mixed: bfloat16 [1024, 4096], P('sp', 'tp')
The draws below stay inside these ranges and needn't reach their ends.
Inputs may be any that keep to these rules, and one draw needn't show every extreme that they name: `routes`: each row names two different experts; in each aligned block of 128 rows no expert is named more than 64 times, a bound that some block reaches.
All inputs are finite; a program needn't handle non-finite values.
Results may differ from the reference program's by a relative error of at most 0.015.
Values may be sent and summed in bfloat16 or wider, within the bound.
No kernel may reach another device: no remote copies, remote signals or barrier semaphores. Data moves between devices by JAX's collectives and lax.ppermute only.
A program may use at most 64 MiB of HBM per device.

```python
import math
import jax
import jax.numpy as jnp
import numpy as np
from jax import lax

D = 4096
HEADS = 16
DH1 = 128
DH2 = 64
FFE = 2048
TOK_DEV = 128
TOKENS = 1024
EXPERTS = 8
CAP = 64
N_SP = 8
N_TP = 4


def head_plan(key):
    slow_share = 0.5
    return jax.random.bernoulli(jax.random.fold_in(key, 17), slow_share, (2, HEADS))


def row_plan(key):
    planted_end = max(1, 3 * TOKENS // 32)
    planted = jnp.arange(TOKENS) < planted_end
    aligned = jax.random.bernoulli(jax.random.fold_in(key, 19), 0.25, (TOKENS,))
    return (planted & aligned, planted & jnp.logical_not(aligned))


def direction(key, group, head_size):
    signs = jax.random.bernoulli(jax.random.fold_in(key, 23 + group), 0.5, (HEADS, head_size))
    return signs.astype(jnp.float32) * 2.0 - 1.0


def noise(key, shape):
    return jnp.clip(jax.random.normal(key, shape, jnp.float32), -5.0, 5.0)


def query_draw(key, group, head_size, salt):
    slow = head_plan(key)[group]
    signs = direction(key, group, head_size)
    strength = min(7.0 / head_size ** 0.5, 1.2)
    base = noise(jax.random.fold_in(key, salt), (TOKENS, HEADS, head_size))
    lifted = base + jnp.where(slow[None, :, None], strength * signs[None], 0.0)
    return lifted.reshape(TOKENS, HEADS * head_size).astype(jnp.bfloat16)


def key_draw(key, group, head_size, salt):
    slow = head_plan(key)[group][None, :, None]
    signs = direction(key, group, head_size)
    aligned, decoy = row_plan(key)
    shape = (TOKENS, HEADS, head_size)
    base = noise(jax.random.fold_in(key, salt), shape)
    sizes = jax.random.uniform(jax.random.fold_in(key, salt + 1), shape, jnp.float32, 0.8, 1.2)
    flips = jax.random.bernoulli(jax.random.fold_in(key, salt + 2), 0.5, shape).astype(jnp.float32) * 2.0 - 1.0
    decoy_rows = 3.0 * sizes * flips
    aligned_rows = signs[None] * sizes
    picked = jnp.where(slow & decoy[:, None, None], decoy_rows, base)
    picked = jnp.where(slow & aligned[:, None, None], aligned_rows, picked)
    return picked.reshape(TOKENS, HEADS * head_size).astype(jnp.bfloat16)


def draw_queries_one(key, part):
    return query_draw(key, 0, DH1, 41)


def draw_queries_two(key, part):
    return query_draw(key, 1, DH2, 51)


def draw_keys_one(key, part):
    return key_draw(key, 0, DH1, 61)


def draw_keys_two(key, part):
    return key_draw(key, 1, DH2, 71)


def draw_key_offset(key, part):
    key_blocks, key_rough, key_low, key_high = jax.random.split(jax.random.fold_in(key, 29), 4)
    slow_heads = head_plan(key)
    aligned, decoy = row_plan(key)
    base_rate = jnp.where(slow_heads, -jnp.log(2.0 * TOKENS), -jnp.log(30.0))
    by_block = jax.random.uniform(key_blocks, (TOKENS // TOK_DEV, 2, HEADS), jnp.float32, -0.7, 0.7)
    by_block = jnp.repeat(by_block, TOK_DEV, axis=0)
    roughness = jax.random.uniform(key_rough, (TOKENS, 2, HEADS), jnp.float32, -0.5, 0.5)
    offsets = base_rate[None].astype(jnp.float32) + by_block + roughness
    decoy_level = jax.random.uniform(key_low, (TOKENS, 2, HEADS), jnp.float32, -12.5, -11.5)
    aligned_level = jax.random.uniform(key_high, (TOKENS, 2, HEADS), jnp.float32, -4.5, -3.5)
    slow = slow_heads[None]
    offsets = jnp.where(slow & decoy[:, None, None], decoy_level, offsets)
    offsets = jnp.where(slow & aligned[:, None, None], aligned_level, offsets)
    return offsets.astype(jnp.bfloat16)


def steps_of(own_key, shape, cuts, least, high):
    def one(dim, blocks):
        steps = jax.random.uniform(jax.random.fold_in(jax.random.fold_in(own_key, 6), dim), (blocks,), jnp.float32, least / len(cuts), high / len(cuts))
        return jnp.repeat(jnp.exp(steps), shape[dim] // blocks).reshape((-1,) + (1,) * (len(shape) - dim - 1))

    factor_of = one(*cuts[0])
    for cut in cuts[1:]:
        factor_of = factor_of * one(*cut)
    return factor_of


def shared_out(rng, own, number, rows, amount, top, reach, slope):
    sequence = jax.random.permutation(rng, amount)
    heavy_load, ordinary = shares(amount, rows * top, reach, slope, True), shares(amount, rows * top, reach, slope, False)
    places = jnp.arange(amount)

    def named(lengths, turn):
        used = int((lengths > 0).sum())
        fixed = max(1, used // 4)
        moved = fixed + (places - fixed + turn * (used - fixed)) % max(1, amount - fixed)
        return jnp.zeros((amount,), jnp.int32).at[sequence[jnp.where(places < fixed, places, moved)]].set(jnp.asarray(lengths, jnp.int32))

    lengths = jnp.where(number % 4 == 0, named(heavy_load, number // 4), named(ordinary, number - number // 4 - 1))
    mixed = jax.random.permutation(jax.random.fold_in(own, 3), amount)
    source_of, sink = mixed[0:amount // 2 * 2:2], mixed[1:amount // 2 * 2:2]
    room = jnp.minimum(lengths[source_of] - 1, reach - lengths[sink]) // 2
    room = jnp.where((source_of == sequence[0]) | (sink == sequence[0]) | (lengths[sink] == 0), 0, jnp.maximum(room, 0))
    moved = jax.random.randint(jax.random.fold_in(own, 4), (amount // 2,), 0, 1 << 20) % (room + 1)
    lengths = lengths.at[source_of].add(-moved).at[sink].add(moved)
    members = jnp.searchsorted(jnp.cumsum(lengths), jnp.arange(rows * top), side="right").astype(jnp.int32)
    listing = members.reshape(top, rows).T
    listing = listing[jax.random.permutation(jax.random.fold_in(own, 1), rows)]
    turn = jax.random.randint(jax.random.fold_in(own, 2), (rows, 1), 0, top)
    return jnp.take_along_axis(listing, (jnp.arange(top)[None, :] + turn) % top, axis=1)


def shares(count, total, bound, slope, full):
    portions = [(1 << 20) // math.isqrt(grade ** slope) + 1 for grade in range(1, count + 1)]
    largest = bound if full else min(bound, max(-(-total // count), total * portions[0] // sum(portions)))
    least = 1 if total - largest >= count - 1 else 0
    holding, rest = [largest] + [least] * (count - 1), total - largest - least * (count - 1)
    while rest > 0:
        candidates = [i for i in range(1, count) if holding[i] < largest] or [i for i in range(1, count) if holding[i] < bound]
        whole, remaining = sum([portions[i] for i in candidates]), rest
        for i in candidates:
            extra = min(bound - holding[i], max(1, remaining * portions[i] // whole), rest)
            holding[i] = holding[i] + extra
            rest = rest - extra
    return np.array(holding)


def centred(key, shape, width, bound, pieces=(), kind=jnp.bfloat16):
    values = jax.random.normal(key, shape, jnp.float32) * width
    if len(pieces) > 0:
        values = steps_of(key, shape, pieces, -0.22, 0.18) * values
    return jnp.clip(values, min=-bound, max=bound).astype(kind)


def setup_inputs(seed: int = 0) -> dict:
    seeds = jax.random.split(jax.random.key(seed), 17)
    queries_one = draw_queries_one(jax.random.fold_in(seeds[16], 71), 0)
    keys_one = draw_keys_one(jax.random.fold_in(seeds[16], 71), 0)
    values_one = centred(seeds[2], (TOKENS, HEADS * DH1), 1.0, 6.0, ((0, 8), (1, 4)))
    queries_two = draw_queries_two(jax.random.fold_in(seeds[16], 71), 0)
    keys_two = draw_keys_two(jax.random.fold_in(seeds[16], 71), 0)
    values_two = centred(seeds[5], (TOKENS, HEADS * DH2), 1.0, 6.0, ((0, 8), (1, 4)))
    key_offset = draw_key_offset(jax.random.fold_in(seeds[16], 71), 0)
    out_one = centred(seeds[7], (HEADS * DH1, D), (HEADS * (DH1 + DH2)) ** -0.5, 0.109375, ((0, 4),))
    out_two = centred(seeds[8], (HEADS * DH2, D), (HEADS * (DH1 + DH2)) ** -0.5, 0.109375, ((0, 4),))
    residual = centred(seeds[9], (TOKENS, D), 1.0, 6.0, ((0, 8), (1, 4)))
    norm_gain = jnp.clip(1.0 + 0.18 * jax.random.normal(seeds[10], (D,), jnp.float32), 0.1, 1.9)
    routes_keys = jax.random.split(jax.random.fold_in(seeds[11], 1), TOKENS // TOK_DEV)
    routes_turns = jax.random.permutation(jax.random.fold_in(seeds[11], 3), TOKENS // TOK_DEV)
    routes = jax.vmap(lambda own, number: shared_out(jax.random.fold_in(seeds[11], 2), own, number, TOK_DEV, EXPERTS, 2, CAP, 2))(routes_keys, routes_turns).reshape((TOKENS, 2))
    route_weight = jnp.clip(0.2 + 0.8 * jax.random.uniform(seeds[12], (TOKENS, 2), jnp.float32) ** steps_of(seeds[12], (TOKENS, 2), ((0, 8),), -0.2, 0.2), 0.2, 1.0)
    expert_gate = centred(seeds[13], (EXPERTS, D, FFE), D ** -0.5, 0.09375, ((0, 8), (2, 4)))
    expert_up = centred(seeds[14], (EXPERTS, D, FFE), D ** -0.5, 0.09375, ((0, 8), (2, 4)))
    expert_down = centred(seeds[15], (EXPERTS, FFE, D), FFE ** -0.5, 0.125, ((0, 8), (2, 4)))
    return {"queries_one": queries_one, "keys_one": keys_one, "values_one": values_one, "queries_two": queries_two, "keys_two": keys_two, "values_two": values_two, "key_offset": key_offset, "out_one": out_one, "out_two": out_two, "residual": residual, "norm_gain": norm_gain, "routes": routes, "route_weight": route_weight, "expert_gate": expert_gate, "expert_up": expert_up, "expert_down": expert_down}


EPS = 1e-06

def stick(query, keys, values, offset, head_size):
    total_len, col_count = query.shape
    head_count = col_count // head_size
    query_heads = query.astype(jnp.float32).reshape(total_len // TOK_DEV, TOK_DEV, head_count, head_size)
    key_heads = keys.astype(jnp.float32).reshape(total_len, head_count, head_size)
    value_heads = values.astype(jnp.float32).reshape(total_len, head_count, head_size)
    bias_rows = offset.astype(jnp.float32).T
    key_pos = jnp.arange(total_len, dtype=jnp.int32)

    def one_block(inputs):
        query_block, block_index = inputs
        scores = jnp.einsum('qhd,khd->hqk', query_block, key_heads) * head_size ** (-0.5) + bias_rows[:, None, :]
        query_pos = block_index * TOK_DEV + jnp.arange(TOK_DEV, dtype=jnp.int32)
        causal = key_pos[None, :] < query_pos[:, None]
        log_beta = jax.nn.log_sigmoid(scores)
        log_rest = jnp.where(causal, jax.nn.log_sigmoid(-scores), 0.0)
        shifted = jnp.pad(log_rest[..., 1:], ((0, 0), (0, 0), (0, 1)))
        carried = lax.cumsum(shifted, axis=2, reverse=True)
        weights = jnp.where(causal, jnp.exp(log_beta + carried), 0.0).astype(jnp.bfloat16)
        weights = lax.optimization_barrier(weights)
        result = jnp.einsum('hqk,khd->qhd', weights.astype(jnp.float32), value_heads)
        return result.reshape(TOK_DEV, col_count).astype(jnp.bfloat16)
    blocks_out = lax.map(one_block, (query_heads, jnp.arange(total_len // TOK_DEV, dtype=jnp.int32)))
    return blocks_out.reshape(total_len, col_count)

def reference(queries_one, keys_one, values_one, queries_two, keys_two, values_two, key_offset, out_one, out_two, residual, norm_gain, routes, route_weight, expert_gate, expert_up, expert_down):
    total_len = residual.shape[0]
    attended_one = stick(queries_one, keys_one, values_one, key_offset[:, 0, :], DH1)
    attended_two = stick(queries_two, keys_two, values_two, key_offset[:, 1, :], DH2)
    per_block = HEADS // N_TP
    heads_one = attended_one.reshape(total_len, N_TP, per_block * DH1)
    heads_two = attended_two.reshape(total_len, N_TP, per_block * DH2)
    proj_one = out_one.reshape(N_TP, per_block * DH1, D)
    proj_two = out_two.reshape(N_TP, per_block * DH2, D)

    def add_partial(tp_index, running):
        partial_value = jnp.dot(lax.dynamic_index_in_dim(heads_one, tp_index, 1, keepdims=False), lax.dynamic_index_in_dim(proj_one, tp_index, 0, keepdims=False), preferred_element_type=jnp.float32)
        partial_value = partial_value + jnp.dot(lax.dynamic_index_in_dim(heads_two, tp_index, 1, keepdims=False), lax.dynamic_index_in_dim(proj_two, tp_index, 0, keepdims=False), preferred_element_type=jnp.float32)
        rounded = lax.optimization_barrier(partial_value.astype(jnp.bfloat16))
        return running + rounded.astype(jnp.float32)
    projected = lax.fori_loop(0, N_TP, add_partial, jnp.zeros((total_len, D), jnp.float32))
    stream = (residual.astype(jnp.float32) + projected).astype(jnp.bfloat16)
    stream_f = stream.astype(jnp.float32)
    normed = (stream_f * lax.rsqrt(lax.optimization_barrier(jnp.mean(stream_f * stream_f, axis=1, keepdims=True)) + EPS) * norm_gain).astype(jnp.bfloat16)
    flat_ids = routes.reshape(-1)
    slot_count = N_SP * CAP

    def one_expert(placed, inputs):
        expert_index, gate_w, up_w, down_w = inputs
        is_routed = flat_ids == expert_index
        picked_rows = jnp.nonzero(is_routed, size=slot_count, fill_value=0)[0]
        is_valid = jnp.arange(slot_count) < jnp.sum(is_routed)
        gathered_rows = normed[picked_rows // 2]
        gate_act = jnp.dot(gathered_rows, gate_w, preferred_element_type=jnp.float32)
        up_act = jnp.dot(gathered_rows, up_w, preferred_element_type=jnp.float32)
        hidden = (jax.nn.silu(gate_act) * up_act).astype(jnp.bfloat16)
        expert_result = jnp.dot(hidden, down_w, preferred_element_type=jnp.float32).astype(jnp.bfloat16)
        expert_result = lax.optimization_barrier(expert_result)
        placed = placed.at[picked_rows].add(jnp.where(is_valid[:, None], expert_result.astype(jnp.float32), 0.0))
        return (placed, None)
    placed, _ = lax.scan(one_expert, jnp.zeros((2 * total_len, D), jnp.float32), (jnp.arange(EXPERTS, dtype=jnp.int32), expert_gate, expert_up, expert_down))
    placed = placed.reshape(total_len, 2, D)
    combined = route_weight[:, 0:1] * placed[:, 0] + route_weight[:, 1:2] * placed[:, 1]
    return (stream_f + combined).astype(jnp.bfloat16)
```

```python
import functools

import jax
import jax.numpy as jnp
from jax import lax
from jax.experimental import pallas as pl
from jax.experimental.pallas import tpu as pltpu
from jax.sharding import PartitionSpec as P

DH1 = 128
DH2 = 64


EPS = 1e-06


def stick_group(query, keys, values, offset, head_size, own_start, key_block):
    row_count = query.shape[0]
    head_count = query.shape[1] // head_size
    query_heads = query.reshape(row_count, head_count, head_size)
    query_pos = own_start + jnp.arange(row_count, dtype=jnp.int32)
    block_count = (own_start + row_count + key_block - 1) // key_block

    def key_step(step_index, state_pair):
        summed, carried = state_pair
        first_key = (block_count - 1 - step_index) * key_block
        key_rows = lax.dynamic_slice_in_dim(keys, first_key, key_block, 0).reshape(
            key_block, head_count, head_size
        )
        value_rows = lax.dynamic_slice_in_dim(values, first_key, key_block, 0).reshape(
            key_block, head_count, head_size
        )
        bias_rows = lax.dynamic_slice_in_dim(offset, first_key, key_block, 0).astype(jnp.float32)
        scores = jnp.einsum(
            "qhd,khd->hqk", query_heads, key_rows, preferred_element_type=jnp.float32
        )
        scores = scores * head_size ** (-0.5) + bias_rows.T[:, None, :]
        key_pos = first_key + jnp.arange(key_block, dtype=jnp.int32)
        causal = key_pos[None, :] < query_pos[:, None]
        log_beta = jax.nn.log_sigmoid(scores)
        log_rest = jnp.where(causal, jax.nn.log_sigmoid(-scores), 0.0)
        shifted = jnp.pad(log_rest[..., 1:], ((0, 0), (0, 0), (0, 1)))
        within = lax.cumsum(shifted, axis=2, reverse=True)
        weights = jnp.where(causal, jnp.exp(log_beta + within + carried[..., None]), 0.0).astype(
            jnp.bfloat16
        )
        summed = summed + jnp.einsum(
            "hqk,khd->hqd", weights, value_rows, preferred_element_type=jnp.float32
        )
        carried = carried + jnp.sum(log_rest, axis=2)
        return (summed, carried)

    start_state = (
        jnp.zeros((head_count, row_count, head_size), jnp.float32),
        jnp.zeros((head_count, row_count), jnp.float32),
    )
    summed, _ = lax.fori_loop(0, block_count, key_step, start_state)
    return summed.transpose(1, 0, 2).reshape(row_count, head_count * head_size).astype(jnp.bfloat16)


def body(
    queries_one,
    keys_one,
    values_one,
    queries_two,
    keys_two,
    values_two,
    key_offset,
    out_one,
    out_two,
    residual,
    norm_gain,
    routes,
    route_weight,
    expert_gate,
    expert_up,
    expert_down,
):
    row_count = queries_one.shape[0]
    spread = lax.axis_size("sp")
    tp_count = lax.axis_size("tp")
    own_start = lax.axis_index("sp") * row_count
    factor = max(1, min(spread, 512 // row_count))
    while spread % factor:
        factor -= 1
    key_block = row_count * factor
    far_k1, far_v1, far_k2, far_v2, far_offset = (
        lax.all_gather(keys_one, "sp", axis=0, tiled=True),
        lax.all_gather(values_one, "sp", axis=0, tiled=True),
        lax.all_gather(keys_two, "sp", axis=0, tiled=True),
        lax.all_gather(values_two, "sp", axis=0, tiled=True),
        lax.all_gather(key_offset, "sp", axis=0, tiled=True),
    )
    attended_one = stick_group(
        queries_one, far_k1, far_v1, far_offset[:, 0, :], DH1, own_start, key_block
    )
    attended_two = stick_group(
        queries_two, far_k2, far_v2, far_offset[:, 1, :], DH2, own_start, key_block
    )
    partial_value = jnp.dot(attended_one, out_one, preferred_element_type=jnp.float32)
    partial_value = partial_value + jnp.dot(
        attended_two, out_two, preferred_element_type=jnp.float32
    )
    columns = residual.shape[1]
    column_start = lax.axis_index("tp") * columns
    resid_full = lax.all_gather(residual, "tp", axis=1, tiled=True)
    projected = lax.psum(partial_value.astype(jnp.bfloat16), "tp").astype(jnp.float32)
    stream = (resid_full.astype(jnp.float32) + projected).astype(jnp.bfloat16)
    stream_f = stream.astype(jnp.float32)
    normed = (
        stream_f * lax.rsqrt(jnp.mean(stream_f * stream_f, axis=1, keepdims=True) + EPS) * norm_gain
    ).astype(jnp.bfloat16)
    stream_own = lax.dynamic_slice_in_dim(stream, column_start, columns, 1)
    capacity = tp_count * ((4 * row_count // spread + tp_count - 1) // tp_count)
    flat_ids = routes.reshape(-1)
    onehot = (flat_ids[:, None] == jnp.arange(spread, dtype=jnp.int32)[None, :]).astype(jnp.int32)
    before = jnp.cumsum(onehot, axis=0) - onehot
    slot_of = flat_ids * capacity + jnp.sum(before * onehot, axis=1)
    chosen = slot_of[:, None] == jnp.arange(spread * capacity, dtype=jnp.int32)[None, :]
    selector = jnp.any(chosen.reshape(row_count, 2, spread * capacity), axis=1).T.astype(
        jnp.bfloat16
    )
    outgoing = jnp.dot(selector, normed, preferred_element_type=jnp.float32).astype(jnp.bfloat16)
    outgoing = outgoing.reshape(spread, capacity, normed.shape[1])
    gate_w = expert_gate[0]
    up_w = expert_up[0]
    down_w = expert_down[0]
    share_size = capacity // tp_count
    own_part = lax.dynamic_slice_in_dim(outgoing, lax.axis_index("tp") * share_size, share_size, 1)
    arrived = lax.all_to_all(own_part, "sp", split_axis=0, concat_axis=0, tiled=True)
    arrived = lax.all_gather(arrived, "tp", axis=1, tiled=True)
    sources, items, _ = arrived.shape
    flat_rows = arrived.reshape(sources * items, arrived.shape[2])
    gate_act = jnp.dot(flat_rows, gate_w, preferred_element_type=jnp.float32)
    up_act = jnp.dot(flat_rows, up_w, preferred_element_type=jnp.float32)
    hidden = (jax.nn.silu(gate_act) * up_act).astype(jnp.bfloat16)
    summed = jnp.dot(
        lax.all_gather(hidden, "tp", axis=1, tiled=True), down_w, preferred_element_type=jnp.float32
    )
    returned = lax.all_to_all(
        summed.astype(jnp.bfloat16).reshape(sources, items, down_w.shape[1]),
        "sp",
        split_axis=0,
        concat_axis=0,
        tiled=True,
    )
    back_rows = returned.reshape(spread * capacity, returned.shape[2])
    picked = jnp.dot(chosen.astype(jnp.bfloat16), back_rows, preferred_element_type=jnp.float32)
    picked = picked.reshape(row_count, 2, back_rows.shape[1])
    combined = route_weight[:, 0:1] * picked[:, 0] + route_weight[:, 1:2] * picked[:, 1]
    return (stream_own.astype(jnp.float32) + combined).astype(jnp.bfloat16)


MIB = 1 << 20
F32 = jnp.float32
BF16 = jnp.bfloat16


def odd(index):
    return (index ^ (index >> 1)) & 1


def vmem():
    return pl.BlockSpec(memory_space=pltpu.VMEM)


def smem():
    return pl.BlockSpec(memory_space=pltpu.SMEM)


def local_call(kernel, name, shapes, inputs, scalars, scratch=(), limit=16):
    return pl.pallas_call(
        kernel,
        name=name,
        out_shape=shapes,
        in_specs=[smem()] * scalars + [vmem()] * (len(inputs) - scalars),
        out_specs=jax.tree.map(lambda _: vmem(), shapes),
        scratch_shapes=list(scratch),
        compiler_params=pltpu.CompilerParams(vmem_limit_bytes=limit * MIB),
    )(*inputs)


def pack_kernel(count, me_ref, q1, k1, v1, q2, k2, v2, offset, *outs):
    wide, slim = outs[:count], outs[count:]
    rows, lanes = q1.shape[0], DH1
    half = rows // 2
    low = lax.broadcasted_iota(jnp.int32, (half, lanes), 1) < DH2
    me = me_ref[0]
    for k in range(count):
        dest = me ^ k
        head = dest >> 1

        @pl.when(odd(dest) == 0)
        def _():
            columns = pl.ds(pl.multiple_of(head * lanes, lanes), lanes)
            for place, source in enumerate((q1, k1, v1)):
                wide[k][place * rows : (place + 1) * rows, :] = source[:, columns]
            wide[k][3 * rows :, :] = jnp.broadcast_to(offset[pl.ds(head, 1), :], (16, rows)).astype(
                BF16
            )

        @pl.when(odd(dest) == 1)
        def _():
            columns = pl.ds(pl.multiple_of((head >> 1) * lanes, lanes), lanes)
            for place, source in enumerate((q2, k2, v2)):
                tile = source[:, columns].astype(F32)
                turned = pltpu.roll(tile, DH2, 1)
                first = jnp.where((head & 1) == 1, turned[:half], tile[:half])
                second = jnp.where((head & 1) == 1, tile[half:], turned[half:])
                slim[k][place * half : (place + 1) * half, :] = jnp.where(
                    low, first, second
                ).astype(BF16)
            slim[k][3 * half :, :] = jnp.broadcast_to(
                offset[pl.ds(count // 2 + head, 1), :], (16, rows)
            ).astype(BF16)


def attend_kernel(count, me_ref, *refs):
    wide, slim, outs = refs[:count], refs[count : 2 * count], refs[2 * count : 3 * count]
    q_all, k_all, v_all, bias_all, o_all = refs[3 * count :]
    lanes = DH1
    rows = outs[0].shape[0]
    half = rows // 2
    me = me_ref[0]
    light = odd(me)
    low = lax.broadcasted_iota(jnp.int32, (half, lanes), 1) < DH2
    for k in range(count):
        source = me ^ k
        place = pl.multiple_of(source * rows, rows)

        @pl.when(light == 0)
        def _():
            for part, target in enumerate((q_all, k_all, v_all)):
                target[pl.ds(place, rows), :] = wide[k][part * rows : (part + 1) * rows, :]
            bias_all[pl.ds(source, 1), :] = wide[k][3 * rows :, :].astype(F32)[0:1]

        @pl.when(light == 1)
        def _():
            shift = (me >> 1) & 1
            for part, target in enumerate((q_all, k_all, v_all)):
                packed = slim[k][part * half : (part + 1) * half, :].astype(F32)
                turned = pltpu.roll(packed, DH2, 1)
                if part < 2:
                    first, second = jnp.where(low, packed, 0.0), jnp.where(low, turned, 0.0)
                else:
                    keep = low ^ (shift == 1)
                    first = jnp.where(keep, jnp.where(shift == 1, turned, packed), 0.0)
                    second = jnp.where(keep, jnp.where(shift == 1, packed, turned), 0.0)
                target[pl.ds(place, half), :] = first.astype(BF16)
                target[pl.ds(place + half, half), :] = second.astype(BF16)
            bias_all[pl.ds(source, 1), :] = slim[k][3 * half :, :].astype(F32)[0:1]

    scale = jnp.where(light == 1, DH2 ** (-0.5), DH1 ** (-0.5)).astype(F32)
    row_at = lax.broadcasted_iota(jnp.int32, (rows, rows), 0)
    col_at = lax.broadcasted_iota(jnp.int32, (rows, rows), 1)
    causal = col_at < row_at
    later = jnp.concatenate(
        [(row_at > col_at).astype(F32), jnp.ones((rows, rows), F32)], axis=1
    ).astype(BF16)
    for query_block in range(count):
        query = q_all[query_block * rows : (query_block + 1) * rows, :]
        carried, total = None, None
        for key_block in range(query_block, -1, -1):
            span = slice(key_block * rows, (key_block + 1) * rows)
            score = lax.dot_general(
                query, k_all[span, :], (((1,), (1,)), ((), ())), preferred_element_type=F32
            )
            score = score * scale + bias_all[key_block : key_block + 1, :]
            log_beta = jnp.minimum(score, 0.0) - jnp.log(1.0 + jnp.exp(-jnp.abs(score)))
            log_rest = log_beta - score
            if key_block == query_block:
                log_rest = jnp.where(causal, log_rest, 0.0)
            coarse = log_rest.astype(BF16)
            fine = (log_rest - coarse.astype(F32)).astype(BF16)
            sums = jnp.dot(coarse, later, preferred_element_type=F32) + jnp.dot(
                fine, later, preferred_element_type=F32
            )
            power = log_beta + sums[:, :rows]
            if carried is not None:
                power = power + carried
            weight = jnp.exp(power)
            if key_block == query_block:
                weight = jnp.where(causal, weight, 0.0)
            added = jnp.dot(weight.astype(BF16), v_all[span, :], preferred_element_type=F32)
            total = added if total is None else total + added
            carried = sums[:, rows:] if carried is None else carried + sums[:, rows:]
        o_all[query_block * rows : (query_block + 1) * rows, :] = total.astype(BF16)
    for k in range(count):
        outs[k][...] = o_all[pl.ds(pl.multiple_of((me ^ k) * rows, rows), rows), :]


def project_kernel(count, moves, me_ref, *refs):
    heads, (w1, w2, out, left) = refs[:count], refs[count:]
    rows, lanes = heads[0].shape
    wide_columns = w1.shape[0]
    me, part = me_ref[0], me_ref[1]
    left[:, wide_columns:] = jnp.zeros((rows, w2.shape[0]), BF16)
    for k in range(count):
        source = me ^ k

        @pl.when(odd(source) == 0)
        def _():
            left[:, pl.ds(pl.multiple_of((source >> 1) * lanes, lanes), lanes)] = heads[k][...]

        @pl.when(odd(source) == 1)
        def _():
            columns = pl.ds(pl.multiple_of(wide_columns + (source >> 2) * lanes, lanes), lanes)
            left[:, columns] = (left[:, columns].astype(F32) + heads[k][...].astype(F32)).astype(
                BF16
            )

    width = out.shape[2]
    for place, move in enumerate(moves):
        columns = pl.ds(pl.multiple_of((part ^ move) * width, width), width)
        value = jnp.dot(left[:, :wide_columns], w1[:, columns], preferred_element_type=F32)
        value = value + jnp.dot(left[:, wide_columns:], w2[:, columns], preferred_element_type=F32)
        out[place] = value.astype(BF16)


def slots_of(routes, me, count, capacity, axis):
    first, second = routes
    tokens = first.shape[1 - axis]
    shape = (count, tokens) if axis == 0 else (tokens, count)
    expert = lax.broadcasted_iota(jnp.int32, shape, axis)
    named = ((expert == first) | (expert == second)).astype(F32)
    row = lax.broadcasted_iota(jnp.int32, (tokens, tokens), 0)
    col = lax.broadcasted_iota(jnp.int32, (tokens, tokens), 1)
    if axis == 0:
        before = jnp.dot(
            named.astype(BF16), (row < col).astype(F32).astype(BF16), preferred_element_type=F32
        )
    else:
        before = jnp.dot(
            (col < row).astype(F32).astype(BF16), named.astype(BF16), preferred_element_type=F32
        )
    found = []
    for choice in (first, second):
        place = jnp.sum(jnp.where(expert == choice, before, 0.0), axis=axis, keepdims=True)
        found.append((choice ^ me) * capacity + place.astype(jnp.int32))
    return found


def select_kernel(count, me_ref, kept, first, second, residual, routes, stream, *outs):
    me = me_ref[0]
    capacity = outs[0].shape[0]
    tokens = residual.shape[0]
    projected = kept[0].astype(F32) + first[...].astype(F32) + second[...].astype(F32)
    value = (residual[...].astype(F32) + projected).astype(BF16)
    stream[...] = value
    found = slots_of((routes[0:1, :], routes[1:2, :]), me, count, capacity, 0)
    slot = lax.broadcasted_iota(jnp.int32, (count * capacity, tokens), 0)
    chosen = ((slot == found[0]) | (slot == found[1])).astype(F32).astype(BF16)
    picked = jnp.dot(chosen, value, preferred_element_type=F32).astype(BF16)
    for k in range(count):
        outs[k][...] = picked[k * capacity : (k + 1) * capacity]


def hidden_kernel(chunks, parts, me_ref, *refs):
    pieces, (gain, gate_w, up_w, out, left) = refs[: chunks * parts], refs[chunks * parts :]
    part = me_ref[1]
    rows, width = pieces[0].shape
    square = jnp.zeros((chunks * rows, 1), F32)
    for move in range(parts):
        columns = pl.ds(pl.multiple_of((part ^ move) * width, width), width)
        for chunk in range(chunks):
            left[chunk * rows : (chunk + 1) * rows, columns] = pieces[chunk * parts + move][...]
        value = left[:, columns].astype(F32)
        square = square + jnp.sum(value * value, axis=1, keepdims=True)
    scale = lax.rsqrt(square * (1.0 / (parts * width)) + EPS)
    gate = up = None
    for piece in range(parts):
        columns = slice(piece * width, (piece + 1) * width)
        normed = (left[:, columns].astype(F32) * scale * gain[:, columns]).astype(BF16)
        more_gate = jnp.dot(normed, gate_w[0, columns, :], preferred_element_type=F32)
        more_up = jnp.dot(normed, up_w[0, columns, :], preferred_element_type=F32)
        gate = more_gate if gate is None else gate + more_gate
        up = more_up if up is None else up + more_up
    out[...] = (gate / (1.0 + jnp.exp(-gate)) * up).astype(BF16)


def down_kernel(chunks, parts, me_ref, *refs):
    pieces, down_w, outs = refs[:parts], refs[parts], refs[parts + 1 :]
    part = me_ref[1]
    depth = pieces[0].shape[1]
    total = None
    for move in range(parts):
        rows = pl.ds(pl.multiple_of((part ^ move) * depth, depth), depth)
        more = jnp.dot(pieces[move][...], down_w[0, rows, :], preferred_element_type=F32)
        total = more if total is None else total + more
    total = total.astype(BF16)
    size = outs[0].shape[0]
    for chunk in range(chunks):
        outs[chunk][...] = total[chunk * size : (chunk + 1) * size]


def mix_kernel(count, me_ref, stream, routes, route_weight, *refs):
    backs, (out, gathered) = refs[:count], refs[count:]
    me = me_ref[0]
    capacity = backs[0].shape[0]
    tokens = stream.shape[0]
    for k in range(count):
        gathered[k * capacity : (k + 1) * capacity, :] = backs[k][...]
    found = slots_of((routes[:, 0:1], routes[:, 1:2]), me, count, capacity, 1)
    slot = lax.broadcasted_iota(jnp.int32, (tokens, count * capacity), 1)
    value = stream[...].astype(F32)
    for choice in range(2):
        chosen = (slot == found[choice]).astype(F32).astype(BF16)
        picked = jnp.dot(chosen, gathered[...], preferred_element_type=F32)
        value = value + route_weight[:, choice : choice + 1] * picked
    out[...] = value.astype(BF16)


def by_heads(
    queries_one, keys_one, values_one, queries_two, keys_two, values_two, key_offset,
    out_one, out_two, residual, norm_gain, routes, route_weight, expert_gate, expert_up, expert_down,
):
    rows = queries_one.shape[0]
    count = lax.axis_size("sp")
    parts = lax.axis_size("tp")
    width = residual.shape[1]
    me = jnp.stack([lax.axis_index("sp"), lax.axis_index("tp")]).astype(jnp.int32)
    order = [k for k in range(count - 1, 0, -1)]

    def swap(value, axis, move, keep=lambda target: True):
        size = lax.axis_size(axis)
        return lax.ppermute(
            value, axis, [(i, i ^ move) for i in range(size) if keep(i ^ move)]
        )

    def shaped(*shape):
        return jax.ShapeDtypeStruct(shape, BF16)

    offset_rows = key_offset.transpose(1, 2, 0).reshape(-1, rows).astype(F32)
    packed = local_call(
        functools.partial(pack_kernel, count),
        "pack",
        [shaped(3 * rows + 16, DH1)] * count + [shaped(3 * rows // 2 + 16, DH1)] * count,
        (me, queries_one, keys_one, values_one, queries_two, keys_two, values_two, offset_rows),
        1,
    )
    wide, slim = list(packed[:count]), list(packed[count:])
    for k in order:
        wide[k] = swap(wide[k], "sp", k, lambda target: odd(target) == 0)
        slim[k] = swap(slim[k], "sp", k, lambda target: odd(target) == 1)
    scratch = [pltpu.VMEM((count * rows, DH1), BF16)] * 3
    scratch += [pltpu.VMEM((count, rows), F32), pltpu.VMEM((count * rows, DH1), BF16)]
    heads = list(
        local_call(
            functools.partial(attend_kernel, count),
            "attend",
            [shaped(rows, DH1)] * count,
            (me, *wide, *slim),
            1,
            scratch,
        )
    )
    for k in order:
        heads[k] = swap(heads[k], "sp", k)

    def projected(moves, name):
        return local_call(
            functools.partial(project_kernel, count, moves),
            name,
            shaped(len(moves), rows, width),
            (me, *heads, out_one, out_two),
            1,
            [pltpu.VMEM((rows, out_one.shape[0] + out_two.shape[0]), BF16)],
            20,
        )

    given = swap(projected((1, 3), "project_sent"), "tp", 1)
    kept = projected((0, 2), "project_kept")
    pair = (kept[1].astype(F32) + given[1].astype(F32)).astype(BF16)
    across = swap(pair, "tp", 2)
    capacity = parts * ((4 * rows // count + parts - 1) // parts)
    stream, *sent = local_call(
        functools.partial(select_kernel, count),
        "select",
        [shaped(rows, width)] + [shaped(capacity, width)] * count,
        (me, kept, given[0], across, residual, routes.T),
        1,
    )
    groups = GROUPS(count)
    pieces = {}
    for group in groups:
        for k in group:
            own = sent[k] if k == 0 else swap(sent[k], "sp", k)
            far = swap(own, "tp", 2)
            pieces[k] = [own, swap(own, "tp", 1), far, swap(far, "tp", 1)]
    gain = norm_gain.reshape(1, -1)
    backs = [None] * count
    for number, group in enumerate(groups):
        size = len(group) * capacity
        hidden = local_call(
            functools.partial(hidden_kernel, len(group), parts),
            "hidden",
            shaped(size, expert_gate.shape[2]),
            (me, *[piece for k in group for piece in pieces[k]], gain, expert_gate, expert_up),
            1,
            [pltpu.VMEM((size, parts * width), BF16)],
            28,
        )
        far = swap(hidden, "tp", 2)
        full = (hidden, swap(hidden, "tp", 1), far, swap(far, "tp", 1))
        results = local_call(
            functools.partial(down_kernel, len(group), parts),
            "down",
            [shaped(capacity, width)] * len(group),
            (me, *full, expert_down),
            1,
            (),
            16,
        )
        for k, result in zip(group, results):
            backs[k] = result if k == 0 else swap(result, "sp", k)
    return local_call(
        functools.partial(mix_kernel, count),
        "mix",
        shaped(rows, width),
        (me, stream, routes, route_weight, *backs),
        1,
        [pltpu.VMEM((count * capacity, width), BF16)],
    )


def GROUPS(count):
    half = count // 2
    return [list(range(half, half + half // 2)), list(range(half + half // 2, count)), list(range(half))]


def layer(*arrays):
    count, parts = lax.axis_size("sp"), lax.axis_size("tp")
    wide, slim = arrays[0].shape[1] // DH1, arrays[3].shape[1] // DH2
    fits = wide == slim and wide + slim == count and count & (count - 1) == 0 and count >= 8
    if fits and parts == 4 and arrays[0].shape[0] == DH1 == 2 * DH2:
        return by_heads(*arrays)
    return body(*arrays)


def solution(mesh):
    return jax.shard_map(
        layer,
        mesh=mesh,
        in_specs=(
            P("sp", "tp"),
            P("sp", "tp"),
            P("sp", "tp"),
            P("sp", "tp"),
            P("sp", "tp"),
            P("sp", "tp"),
            P("sp", None, "tp"),
            P("tp", None),
            P("tp", None),
            P("sp", "tp"),
            P(),
            P("sp", None),
            P("sp", None),
            P("sp", None, "tp"),
            P("sp", None, "tp"),
            P("sp", None, "tp"),
        ),
        out_specs=P("sp", "tp"),
        check_vma=False,
    )
```

```python
import functools

import jax
import jax.numpy as jnp
from jax import lax
from jax.experimental import pallas as pl
from jax.experimental.pallas import tpu as pltpu
from jax.sharding import PartitionSpec as P

DH1 = 128
DH2 = 64


EPS = 1e-06


def stick_group(query, keys, values, offset, head_size, own_start, key_block):
    row_count = query.shape[0]
    head_count = query.shape[1] // head_size
    query_heads = query.reshape(row_count, head_count, head_size)
    query_pos = own_start + jnp.arange(row_count, dtype=jnp.int32)
    block_count = (own_start + row_count + key_block - 1) // key_block

    def key_step(step_index, state_pair):
        summed, carried = state_pair
        first_key = (block_count - 1 - step_index) * key_block
        key_rows = lax.dynamic_slice_in_dim(keys, first_key, key_block, 0).reshape(
            key_block, head_count, head_size
        )
        value_rows = lax.dynamic_slice_in_dim(values, first_key, key_block, 0).reshape(
            key_block, head_count, head_size
        )
        bias_rows = lax.dynamic_slice_in_dim(offset, first_key, key_block, 0).astype(jnp.float32)
        scores = jnp.einsum(
            "qhd,khd->hqk", query_heads, key_rows, preferred_element_type=jnp.float32
        )
        scores = scores * head_size ** (-0.5) + bias_rows.T[:, None, :]
        key_pos = first_key + jnp.arange(key_block, dtype=jnp.int32)
        causal = key_pos[None, :] < query_pos[:, None]
        log_beta = jax.nn.log_sigmoid(scores)
        log_rest = jnp.where(causal, jax.nn.log_sigmoid(-scores), 0.0)
        shifted = jnp.pad(log_rest[..., 1:], ((0, 0), (0, 0), (0, 1)))
        within = lax.cumsum(shifted, axis=2, reverse=True)
        weights = jnp.where(causal, jnp.exp(log_beta + within + carried[..., None]), 0.0).astype(
            jnp.bfloat16
        )
        summed = summed + jnp.einsum(
            "hqk,khd->hqd", weights, value_rows, preferred_element_type=jnp.float32
        )
        carried = carried + jnp.sum(log_rest, axis=2)
        return (summed, carried)

    start_state = (
        jnp.zeros((head_count, row_count, head_size), jnp.float32),
        jnp.zeros((head_count, row_count), jnp.float32),
    )
    summed, _ = lax.fori_loop(0, block_count, key_step, start_state)
    return summed.transpose(1, 0, 2).reshape(row_count, head_count * head_size).astype(jnp.bfloat16)


def body(
    queries_one,
    keys_one,
    values_one,
    queries_two,
    keys_two,
    values_two,
    key_offset,
    out_one,
    out_two,
    residual,
    norm_gain,
    routes,
    route_weight,
    expert_gate,
    expert_up,
    expert_down,
):
    row_count = queries_one.shape[0]
    spread = lax.axis_size("sp")
    tp_count = lax.axis_size("tp")
    own_start = lax.axis_index("sp") * row_count
    factor = max(1, min(spread, 512 // row_count))
    while spread % factor:
        factor -= 1
    key_block = row_count * factor
    far_k1, far_v1, far_k2, far_v2, far_offset = (
        lax.all_gather(keys_one, "sp", axis=0, tiled=True),
        lax.all_gather(values_one, "sp", axis=0, tiled=True),
        lax.all_gather(keys_two, "sp", axis=0, tiled=True),
        lax.all_gather(values_two, "sp", axis=0, tiled=True),
        lax.all_gather(key_offset, "sp", axis=0, tiled=True),
    )
    attended_one = stick_group(
        queries_one, far_k1, far_v1, far_offset[:, 0, :], DH1, own_start, key_block
    )
    attended_two = stick_group(
        queries_two, far_k2, far_v2, far_offset[:, 1, :], DH2, own_start, key_block
    )
    partial_value = jnp.dot(attended_one, out_one, preferred_element_type=jnp.float32)
    partial_value = partial_value + jnp.dot(
        attended_two, out_two, preferred_element_type=jnp.float32
    )
    columns = residual.shape[1]
    column_start = lax.axis_index("tp") * columns
    resid_full = lax.all_gather(residual, "tp", axis=1, tiled=True)
    projected = lax.psum(partial_value.astype(jnp.bfloat16), "tp").astype(jnp.float32)
    stream = (resid_full.astype(jnp.float32) + projected).astype(jnp.bfloat16)
    stream_f = stream.astype(jnp.float32)
    normed = (
        stream_f * lax.rsqrt(jnp.mean(stream_f * stream_f, axis=1, keepdims=True) + EPS) * norm_gain
    ).astype(jnp.bfloat16)
    stream_own = lax.dynamic_slice_in_dim(stream, column_start, columns, 1)
    capacity = tp_count * ((4 * row_count // spread + tp_count - 1) // tp_count)
    flat_ids = routes.reshape(-1)
    onehot = (flat_ids[:, None] == jnp.arange(spread, dtype=jnp.int32)[None, :]).astype(jnp.int32)
    before = jnp.cumsum(onehot, axis=0) - onehot
    slot_of = flat_ids * capacity + jnp.sum(before * onehot, axis=1)
    chosen = slot_of[:, None] == jnp.arange(spread * capacity, dtype=jnp.int32)[None, :]
    selector = jnp.any(chosen.reshape(row_count, 2, spread * capacity), axis=1).T.astype(
        jnp.bfloat16
    )
    outgoing = jnp.dot(selector, normed, preferred_element_type=jnp.float32).astype(jnp.bfloat16)
    outgoing = outgoing.reshape(spread, capacity, normed.shape[1])
    gate_w = expert_gate[0]
    up_w = expert_up[0]
    down_w = expert_down[0]
    share_size = capacity // tp_count
    own_part = lax.dynamic_slice_in_dim(outgoing, lax.axis_index("tp") * share_size, share_size, 1)
    arrived = lax.all_to_all(own_part, "sp", split_axis=0, concat_axis=0, tiled=True)
    arrived = lax.all_gather(arrived, "tp", axis=1, tiled=True)
    sources, items, _ = arrived.shape
    flat_rows = arrived.reshape(sources * items, arrived.shape[2])
    gate_act = jnp.dot(flat_rows, gate_w, preferred_element_type=jnp.float32)
    up_act = jnp.dot(flat_rows, up_w, preferred_element_type=jnp.float32)
    hidden = (jax.nn.silu(gate_act) * up_act).astype(jnp.bfloat16)
    summed = jnp.dot(
        lax.all_gather(hidden, "tp", axis=1, tiled=True), down_w, preferred_element_type=jnp.float32
    )
    returned = lax.all_to_all(
        summed.astype(jnp.bfloat16).reshape(sources, items, down_w.shape[1]),
        "sp",
        split_axis=0,
        concat_axis=0,
        tiled=True,
    )
    back_rows = returned.reshape(spread * capacity, returned.shape[2])
    picked = jnp.dot(chosen.astype(jnp.bfloat16), back_rows, preferred_element_type=jnp.float32)
    picked = picked.reshape(row_count, 2, back_rows.shape[1])
    combined = route_weight[:, 0:1] * picked[:, 0] + route_weight[:, 1:2] * picked[:, 1]
    return (stream_own.astype(jnp.float32) + combined).astype(jnp.bfloat16)


MIB = 1 << 20
F32 = jnp.float32
BF16 = jnp.bfloat16


def vmem():
    return pl.BlockSpec(memory_space=pltpu.VMEM)


def smem():
    return pl.BlockSpec(memory_space=pltpu.SMEM)


def far_memory():
    return pl.BlockSpec(memory_space=pltpu.HBM)


def local_call(kernel, name, shapes, inputs, scalars, scratch=(), limit=16, far=0, tail=0):
    near = len(inputs) - scalars - far - tail
    distant = set(range(scalars, scalars + far)) | set(range(len(inputs) - tail, len(inputs)))
    inputs = [
        pltpu.with_memory_space_constraint(value, pltpu.HBM) if place in distant else value
        for place, value in enumerate(inputs)
    ]
    return pl.pallas_call(
        kernel,
        name=name,
        out_shape=shapes,
        in_specs=[smem()] * scalars + [far_memory()] * far + [vmem()] * near + [far_memory()] * tail,
        out_specs=jax.tree.map(lambda _: vmem(), shapes),
        scratch_shapes=list(scratch),
        compiler_params=pltpu.CompilerParams(vmem_limit_bytes=limit * MIB),
    )(*inputs)


def pack_kernel(planes, me_ref, q1, k1, v1, q2, k2, v2, offset, *refs):
    outs, staged, ready = refs[:planes], refs[planes:-1], refs[-1]
    copies = [
        pltpu.make_async_copy(source, target, ready.at[place])
        for place, (source, target) in enumerate(zip((q1, k1, v1, q2, k2, v2), staged))
    ]
    for copy in copies:
        copy.start()
    for copy in copies:
        copy.wait()
    rows, lanes = q1.shape[0], DH1
    half = rows // 2
    low = lax.broadcasted_iota(jnp.int32, (half, lanes), 1) < DH2
    mine = me_ref[0] >> 1
    sq1, sk1, sv1, sq2, sk2, sv2 = staged
    for k in range(planes):
        head = mine ^ k
        columns = pl.ds(pl.multiple_of(head * lanes, lanes), lanes)
        at = 0
        for source in (sk1, sv1):
            outs[k][at : at + rows, :] = source[:, columns]
            at += rows
        pair = pl.ds(pl.multiple_of((head >> 1) * lanes, lanes), lanes)

        def squeezed(source):
            tile = source[:, pair].astype(F32)
            turned = pltpu.roll(tile, DH2, 1)
            first = jnp.where((head & 1) == 1, turned[:half], tile[:half])
            second = jnp.where((head & 1) == 1, tile[half:], turned[half:])
            return jnp.where(low, first, second).astype(BF16)

        for source in (sk2, sv2):
            outs[k][at : at + half, :] = squeezed(source)
            at += half
        bias = jnp.concatenate(
            [
                jnp.broadcast_to(offset[pl.ds(head, 1), :], (8, rows)),
                jnp.broadcast_to(offset[pl.ds(planes + head, 1), :], (8, rows)),
            ],
            axis=0,
        )
        outs[k][at : at + 16, :] = bias.astype(BF16)
        at += 16
        outs[k][at : at + rows, :] = sq1[:, columns]
        outs[k][at + rows :, :] = squeezed(sq2)


def spread_out(packed, shifted):
    half, lanes = packed.shape
    low = lax.broadcasted_iota(jnp.int32, (half, lanes), 1) < DH2
    packed = packed.astype(F32)
    turned = pltpu.roll(packed, DH2, 1)
    if shifted is None:
        return jnp.where(low, packed, 0.0), jnp.where(low, turned, 0.0)
    keep = low ^ (shifted == 1)
    first = jnp.where(keep, jnp.where(shifted == 1, turned, packed), 0.0)
    second = jnp.where(keep, jnp.where(shifted == 1, packed, turned), 0.0)
    return first, second


def attend_kernel(planes, me_ref, *refs):
    own, other, (w1, w2) = refs[:planes], refs[planes : 2 * planes], refs[2 * planes : 2 * planes + 2]
    refs = refs[2 * planes + 2 :]
    outs, (w1_near, w2_near), scratch = refs[:planes], refs[planes : planes + 2], refs[planes + 2 :]
    q_one, k_one, v_one, q_two, k_two, v_two, bias, o_one, o_two, ready = scratch
    copies = [
        pltpu.make_async_copy(w1, w1_near, ready.at[0]),
        pltpu.make_async_copy(w2, w2_near, ready.at[1]),
    ]
    for copy in copies:
        copy.start()
    lanes = DH1
    rows = lanes
    half = rows // 2
    mine, side = me_ref[0] >> 1, me_ref[0] & 1
    for k in range(planes):
        plane = mine ^ k
        for pack, column in ((own[k], side), (other[k], 1 - side)):
            place = pl.multiple_of((2 * plane + column) * rows, rows)
            k_one[pl.ds(place, rows), :] = pack[:rows, :]
            v_one[pl.ds(place, rows), :] = pack[rows : 2 * rows, :]
            at = 2 * rows
            for target in (k_two, v_two):
                first, second = spread_out(pack[at : at + half, :], None)
                target[pl.ds(place, half), :] = first.astype(BF16)
                target[pl.ds(place + half, half), :] = second.astype(BF16)
                at += half
            offsets = pack[at : at + 16, :].astype(F32)
            bias[pl.ds(2 * plane + column, 1), :] = offsets[0:1]
            bias[pl.ds(2 * (planes + plane) + column, 1), :] = offsets[8:9]
        at = 3 * rows + 16
        place = pl.multiple_of(plane * rows, rows)
        q_one[pl.ds(place, rows), :] = own[k][at : at + rows, :]
        first, second = spread_out(own[k][at + rows :, :], None)
        q_two[pl.ds(place, half), :] = first.astype(BF16)
        q_two[pl.ds(place + half, half), :] = second.astype(BF16)

    span = 2 * rows
    causal = lax.broadcasted_iota(jnp.int32, (rows, span), 1) < (
        lax.broadcasted_iota(jnp.int32, (rows, span), 0) + side * rows
    )
    later = jnp.concatenate(
        [
            (
                lax.broadcasted_iota(jnp.int32, (span, span), 0)
                > lax.broadcasted_iota(jnp.int32, (span, span), 1)
            ).astype(F32),
            jnp.ones((span, rows), F32),
        ],
        axis=1,
    ).astype(BF16)
    for group, (queries, keys, values, out, size) in enumerate(
        ((q_one, k_one, v_one, o_one, DH1), (q_two, k_two, v_two, o_two, DH2))
    ):
        for plane in range(planes):
            query = queries[plane * rows : (plane + 1) * rows, :]
            carried, total = None, None
            for block in range(plane, -1, -1):
                part = slice(block * span, (block + 1) * span)
                score = lax.dot_general(
                    query, keys[part, :], (((1,), (1,)), ((), ())), preferred_element_type=F32
                )
                at = 2 * (group * planes + block)
                score = score * size ** (-0.5) + jnp.concatenate(
                    [bias[at : at + 1, :], bias[at + 1 : at + 2, :]], axis=1
                )
                log_beta = jnp.minimum(score, 0.0) - jnp.log(1.0 + jnp.exp(-jnp.abs(score)))
                log_rest = log_beta - score
                if block == plane:
                    log_rest = jnp.where(causal, log_rest, 0.0)
                coarse = log_rest.astype(BF16)
                fine = (log_rest - coarse.astype(F32)).astype(BF16)
                sums = jnp.dot(coarse, later, preferred_element_type=F32) + jnp.dot(
                    fine, later, preferred_element_type=F32
                )
                power = log_beta + sums[:, :span]
                if carried is not None:
                    power = power + jnp.concatenate([carried, carried], axis=1)
                weight = jnp.exp(power)
                if block == plane:
                    weight = jnp.where(causal, weight, 0.0)
                added = jnp.dot(weight.astype(BF16), values[part, :], preferred_element_type=F32)
                total = added if total is None else total + added
                carried = sums[:, span:] if carried is None else carried + sums[:, span:]
            if group == 0:
                out[plane * rows : (plane + 1) * rows, :] = total.astype(BF16)
            else:
                low = lax.broadcasted_iota(jnp.int32, (half, lanes), 1) < DH2
                turned = pltpu.roll(total, DH2, 1)
                out[plane * half : (plane + 1) * half, :] = jnp.where(
                    low, total[:half], turned[half:]
                ).astype(BF16)
    for k in range(planes):
        plane = mine ^ k
        outs[k][:rows, :] = o_one[pl.ds(pl.multiple_of(plane * rows, rows), rows), :]
        outs[k][rows:, :] = o_two[pl.ds(pl.multiple_of(plane * half, half), half), :]
    for copy in copies:
        copy.wait()


def project_kernel(planes, moves, me_ref, *refs):
    heads, (w1, w2, out, left) = refs[:planes], refs[planes:]
    rows, lanes = out.shape[1], DH1
    half = rows // 2
    wide_columns = w1.shape[0]
    mine, part = me_ref[0] >> 1, me_ref[1]
    left[:, wide_columns:] = jnp.zeros((rows, w2.shape[0]), BF16)
    for k in range(planes):
        head = mine ^ k
        left[:, pl.ds(pl.multiple_of(head * lanes, lanes), lanes)] = heads[k][:rows, :]
        columns = pl.ds(pl.multiple_of(wide_columns + (head >> 1) * lanes, lanes), lanes)
        first, second = spread_out(heads[k][rows:, :], head & 1)
        left[:half, columns] = (left[:half, columns].astype(F32) + first).astype(BF16)
        left[half:, columns] = (left[half:, columns].astype(F32) + second).astype(BF16)
    width = out.shape[2]
    for place, move in enumerate(moves):
        columns = pl.ds(pl.multiple_of((part ^ move) * width, width), width)
        value = jnp.dot(left[:, :wide_columns], w1[:, columns], preferred_element_type=F32)
        value = value + jnp.dot(left[:, wide_columns:], w2[:, columns], preferred_element_type=F32)
        out[place] = value.astype(BF16)


def slots_of(routes, me, count, capacity, axis):
    first, second = routes
    tokens = first.shape[1 - axis]
    shape = (count, tokens) if axis == 0 else (tokens, count)
    expert = lax.broadcasted_iota(jnp.int32, shape, axis)
    named = ((expert == first) | (expert == second)).astype(F32)
    row = lax.broadcasted_iota(jnp.int32, (tokens, tokens), 0)
    col = lax.broadcasted_iota(jnp.int32, (tokens, tokens), 1)
    if axis == 0:
        before = jnp.dot(
            named.astype(BF16), (row < col).astype(F32).astype(BF16), preferred_element_type=F32
        )
    else:
        before = jnp.dot(
            (col < row).astype(F32).astype(BF16), named.astype(BF16), preferred_element_type=F32
        )
    found = []
    for choice in (first, second):
        place = jnp.sum(jnp.where(expert == choice, before, 0.0), axis=axis, keepdims=True)
        found.append((choice ^ me) * capacity + place.astype(jnp.int32))
    return found


def select_kernel(count, me_ref, kept, first, second, residual, routes, stream, *outs):
    me = me_ref[0]
    capacity = outs[0].shape[0]
    tokens = residual.shape[0]
    projected = kept[0].astype(F32) + first[...].astype(F32) + second[...].astype(F32)
    value = (residual[...].astype(F32) + projected).astype(BF16)
    stream[...] = value
    found = slots_of((routes[0:1, :], routes[1:2, :]), me, count, capacity, 0)
    slot = lax.broadcasted_iota(jnp.int32, (count * capacity, tokens), 0)
    chosen = ((slot == found[0]) | (slot == found[1])).astype(F32).astype(BF16)
    picked = jnp.dot(chosen, value, preferred_element_type=F32).astype(BF16)
    for k in range(count):
        outs[k][...] = picked[k * capacity : (k + 1) * capacity]


def hidden_kernel(chunks, parts, me_ref, *refs):
    pieces, (gain, gate_w, up_w, out, left) = refs[: chunks * parts], refs[chunks * parts :]
    part = me_ref[1]
    rows, width = pieces[0].shape
    square = jnp.zeros((chunks * rows, 1), F32)
    for move in range(parts):
        columns = pl.ds(pl.multiple_of((part ^ move) * width, width), width)
        for chunk in range(chunks):
            left[chunk * rows : (chunk + 1) * rows, columns] = pieces[chunk * parts + move][...]
        value = left[:, columns].astype(F32)
        square = square + jnp.sum(value * value, axis=1, keepdims=True)
    scale = lax.rsqrt(square * (1.0 / (parts * width)) + EPS)
    gate = up = None
    for piece in range(parts):
        columns = slice(piece * width, (piece + 1) * width)
        normed = (left[:, columns].astype(F32) * scale * gain[:, columns]).astype(BF16)
        more_gate = jnp.dot(normed, gate_w[0, columns, :], preferred_element_type=F32)
        more_up = jnp.dot(normed, up_w[0, columns, :], preferred_element_type=F32)
        gate = more_gate if gate is None else gate + more_gate
        up = more_up if up is None else up + more_up
    out[...] = (gate / (1.0 + jnp.exp(-gate)) * up).astype(BF16)


def down_kernel(chunks, parts, me_ref, *refs):
    pieces, down_w, outs = refs[:parts], refs[parts], refs[parts + 1 :]
    part = me_ref[1]
    depth = pieces[0].shape[1]
    total = None
    for move in range(parts):
        rows = pl.ds(pl.multiple_of((part ^ move) * depth, depth), depth)
        more = jnp.dot(pieces[move][...], down_w[0, rows, :], preferred_element_type=F32)
        total = more if total is None else total + more
    total = total.astype(BF16)
    size = outs[0].shape[0]
    for chunk in range(chunks):
        outs[chunk][...] = total[chunk * size : (chunk + 1) * size]


def mix_kernel(count, me_ref, stream, routes, route_weight, *refs):
    backs, (out, gathered) = refs[:count], refs[count:]
    me = me_ref[0]
    capacity = backs[0].shape[0]
    tokens = stream.shape[0]
    for k in range(count):
        gathered[k * capacity : (k + 1) * capacity, :] = backs[k][...]
    found = slots_of((routes[:, 0:1], routes[:, 1:2]), me, count, capacity, 1)
    slot = lax.broadcasted_iota(jnp.int32, (tokens, count * capacity), 1)
    value = stream[...].astype(F32)
    for choice in range(2):
        chosen = (slot == found[choice]).astype(F32).astype(BF16)
        picked = jnp.dot(chosen, gathered[...], preferred_element_type=F32)
        value = value + route_weight[:, choice : choice + 1] * picked
    out[...] = value.astype(BF16)


def by_heads(
    queries_one, keys_one, values_one, queries_two, keys_two, values_two, key_offset,
    out_one, out_two, residual, norm_gain, routes, route_weight, expert_gate, expert_up, expert_down,
):
    rows = queries_one.shape[0]
    count = lax.axis_size("sp")
    parts = lax.axis_size("tp")
    width = residual.shape[1]
    me = jnp.stack([lax.axis_index("sp"), lax.axis_index("tp")]).astype(jnp.int32)
    order = [k for k in range(count - 1, 0, -1)]

    def swap(value, axis, move, keep=lambda target: True):
        size = lax.axis_size(axis)
        return lax.ppermute(
            value, axis, [(i, i ^ move) for i in range(size) if keep(i ^ move)]
        )

    def shaped(*shape):
        return jax.ShapeDtypeStruct(shape, BF16)

    planes = count // 2
    far_first = sorted(range(1, planes), reverse=True)
    offset_rows = key_offset.transpose(1, 2, 0).reshape(-1, rows).astype(F32)
    sources = (queries_one, keys_one, values_one, queries_two, keys_two, values_two)
    own = list(
        local_call(
            functools.partial(pack_kernel, planes),
            "pack",
            [shaped(9 * rows // 2 + 16, DH1)] * planes,
            (me, *sources, offset_rows),
            1,
            [pltpu.VMEM(source.shape, BF16) for source in sources]
            + [pltpu.SemaphoreType.DMA((len(sources),))],
            far=len(sources),
        )
    )
    keyed = 3 * rows + 16
    other = [None] * planes
    for k in far_first:
        own[k] = swap(own[k], "sp", 2 * k)
    for k in range(planes):
        other[k] = swap(own[k][:keyed], "sp", 1)
    scratch = [pltpu.VMEM((size * rows, DH1), BF16) for size in (planes, count, count)] * 2
    scratch += [pltpu.VMEM((2 * count, rows), F32), pltpu.VMEM((planes * rows, DH1), BF16)]
    scratch += [pltpu.VMEM((planes * rows // 2, DH1), BF16), pltpu.SemaphoreType.DMA((2,))]
    *heads, w1_near, w2_near = local_call(
        functools.partial(attend_kernel, planes),
        "attend",
        [shaped(3 * rows // 2, DH1)] * planes + [shaped(*out_one.shape), shaped(*out_two.shape)],
        (me, *own, *other, out_one, out_two),
        1,
        scratch,
        20,
        tail=2,
    )
    for k in far_first:
        heads[k] = swap(heads[k], "sp", 2 * k)

    def projected(moves, name):
        return local_call(
            functools.partial(project_kernel, planes, moves),
            name,
            shaped(len(moves), rows, width),
            (me, *heads, w1_near, w2_near),
            1,
            [pltpu.VMEM((rows, out_one.shape[0] + out_two.shape[0]), BF16)],
            20,
        )

    given = swap(projected((1, 3), "project_sent"), "tp", 1)
    kept = projected((0, 2), "project_kept")
    pair = (kept[1].astype(F32) + given[1].astype(F32)).astype(BF16)
    across = swap(pair, "tp", 2)
    capacity = parts * ((4 * rows // count + parts - 1) // parts)
    stream, *sent = local_call(
        functools.partial(select_kernel, count),
        "select",
        [shaped(rows, width)] + [shaped(capacity, width)] * count,
        (me, kept, given[0], across, residual, routes.T),
        1,
    )
    groups = GROUPS(count)
    pieces = {}
    for group in groups:
        for k in group:
            own = sent[k] if k == 0 else swap(sent[k], "sp", k)
            far = swap(own, "tp", 2)
            pieces[k] = [own, swap(own, "tp", 1), far, swap(far, "tp", 1)]
    gain = norm_gain.reshape(1, -1)
    backs = [None] * count
    for number, group in enumerate(groups):
        size = len(group) * capacity
        hidden = local_call(
            functools.partial(hidden_kernel, len(group), parts),
            "hidden",
            shaped(size, expert_gate.shape[2]),
            (me, *[piece for k in group for piece in pieces[k]], gain, expert_gate, expert_up),
            1,
            [pltpu.VMEM((size, parts * width), BF16)],
            28,
        )
        far = swap(hidden, "tp", 2)
        full = (hidden, swap(hidden, "tp", 1), far, swap(far, "tp", 1))
        results = local_call(
            functools.partial(down_kernel, len(group), parts),
            "down",
            [shaped(capacity, width)] * len(group),
            (me, *full, expert_down),
            1,
            (),
            16,
        )
        for k, result in zip(group, results):
            backs[k] = result if k == 0 else swap(result, "sp", k)
    return local_call(
        functools.partial(mix_kernel, count),
        "mix",
        shaped(rows, width),
        (me, stream, routes, route_weight, *backs),
        1,
        [pltpu.VMEM((count * capacity, width), BF16)],
    )


def GROUPS(count):
    half = count // 2
    return [list(range(half, half + half // 2)), list(range(half + half // 2, count)), list(range(half))]


def layer(*arrays):
    count, parts = lax.axis_size("sp"), lax.axis_size("tp")
    wide, slim = arrays[0].shape[1] // DH1, arrays[3].shape[1] // DH2
    fits = wide == slim and wide + slim == count and count & (count - 1) == 0 and count >= 8
    if fits and parts == 4 and arrays[0].shape[0] == DH1 == 2 * DH2:
        return by_heads(*arrays)
    return body(*arrays)


def solution(mesh):
    return jax.shard_map(
        layer,
        mesh=mesh,
        in_specs=(
            P("sp", "tp"),
            P("sp", "tp"),
            P("sp", "tp"),
            P("sp", "tp"),
            P("sp", "tp"),
            P("sp", "tp"),
            P("sp", None, "tp"),
            P("tp", None),
            P("tp", None),
            P("sp", "tp"),
            P(),
            P("sp", None),
            P("sp", None),
            P("sp", None, "tp"),
            P("sp", None, "tp"),
            P("sp", None, "tp"),
        ),
        out_specs=P("sp", "tp"),
        check_vma=False,
    )
```
